256 devices in a mesh: ep: 64 (over z, x, core), tp: 4 (over y).
Axes of the slice: x: 4, y: 4, z: 8, core: 2. Of those that a mesh axis runs over, the one named last changes fastest.
Arguments:
- mix_input: bfloat16 [65536, 1024], P(('ep', 'tp')), may hold values from -6 to 6
- pool_weight: bfloat16 [8, 128, 128], replicated, may hold values from -0.5 to 0.5
- pool_scale: float32 [1024], replicated, may hold values from 0.1 to 1.9
- out_weight: bfloat16 [1024, 2048], replicated, may hold values from -0.1875 to 0.1875
- moe_input: bfloat16 [8192, 2048], P('ep'), may hold values from -6 to 6
- moe_gain: float32 [2048], replicated, may hold values from 0.1 to 1.9
- group_router: bfloat16 [2048, 4], replicated, may hold values from -0.125 to 0.125
- inner_router: bfloat16 [2048, 64], replicated, may hold values from -0.125 to 0.125
- group_pick: int32 [8192], P('ep'), may hold values from 0 to 3
- inner_pick: int32 [8192, 2], P('ep'), may hold values from 0 to 15, all different within a row
- gate_weight: bfloat16 [64, 2048, 1024], P('ep', None, 'tp'), may hold values from -0.125 to 0.125
- up_weight: bfloat16 [64, 2048, 1024], P('ep', None, 'tp'), may hold values from -0.125 to 0.125
- down_weight: bfloat16 [64, 1024, 2048], P('ep', 'tp'), may hold values from -0.1875 to 0.1875
Outputs:
- mix_out: bfloat16 [65536, 2048], P(('ep', 'tp'))
- moe_out: bfloat16 [8192, 2048], P('ep', 'tp')
The draws below stay inside these ranges and needn't reach their ends.
All inputs are finite; a program needn't handle non-finite values.
Results may differ from the reference program's by a relative error of at most 0.011.
Values may be sent and summed in bfloat16 or wider, within the bound.
A program may use at most 64 MiB of HBM per device.

```python
import math
import jax
import jax.numpy as jnp
import numpy as np
from jax import lax

D = 2048
FF = 1024
POOL_DIM = 128
POOL_GROUPS = 8
GROUPS = 4
TOPK = 2
WINDOW_MAX = 16
TOK_MOE = 128
D_POOL = 1024
EXPERTS = 64
EPG = 16
CAP = 8
FF_PART = 256
TOKENS_MIX = 65536
TOKENS_MOE = 8192
N_EP = 64
N_TP = 4


def touch_ends(entries, own_key, smallest, top_value):
    dims = entries.shape
    spot = [jax.random.randint(jax.random.fold_in(own_key, axis), (), 0, dims[axis]) for axis in range(len(dims))]
    entries = entries.at[tuple(spot)].set(smallest)
    longest = dims.index(max(dims))
    spot[longest] = (spot[longest] + 1) % dims[longest]
    return entries.at[tuple(spot)].set(top_value)


def shard_levels(stream_key, shape, cuts, smallest, largest):
    factor_of = 1.0
    for dim, parts in cuts:
        steps = jax.random.uniform(jax.random.fold_in(jax.random.fold_in(stream_key, 6), dim), (parts,), jnp.float32, smallest / len(cuts), largest / len(cuts))
        factor_of = factor_of * jnp.repeat(jnp.exp(steps), shape[dim] // parts).reshape((-1,) + (1,) * (len(shape) - 1 - dim))
    return factor_of


def rank_table(count, slope):
    portions = [(1 << 20) // math.isqrt(grade ** slope) + 1 for grade in range(1, count + 1)]
    deviation = 1 + sum(portions) // (1 << 30)
    return np.cumsum(np.array([max(1, weight // deviation) for weight in portions]))


def skewed_ids(stream_key, dims, amount, skew):
    table = rank_table(amount, skew)
    pick = jax.random.randint(jax.random.fold_in(stream_key, 1), dims, 0, int(table[amount - 1]))
    rank = jnp.searchsorted(jnp.asarray(table, jnp.int32), pick, side="right")
    return jax.random.permutation(jax.random.fold_in(stream_key, 2), amount)[rank].astype(jnp.int32)


def distinct(stream_key, rows, amount, top, lift):
    order = jax.random.permutation(jax.random.fold_in(stream_key, 1), amount)
    favour = order
    for power in range(3):
        favour = favour * favour // amount
    favour = favour * lift // amount
    lots = jax.random.randint(jax.random.fold_in(stream_key, 2), (rows, amount), 0, 4096) + favour
    fixed_rows = jax.random.permutation(jax.random.fold_in(stream_key, 3), rows)[jnp.arange(amount) % rows]
    lots = jnp.where(jnp.arange(rows)[:, None] == fixed_rows[None, :], 1 << 14, lots)
    score = lots * amount + jnp.arange(amount)
    return lax.top_k(score.astype(jnp.int32), top)[1].astype(jnp.int32)


def gaussian(own_key, shape, scale, limit, shards=(), held_as=jnp.bfloat16):
    entries = scale * jax.random.normal(own_key, shape, jnp.float32)
    if shards:
        entries = entries * shard_levels(own_key, shape, shards, -0.22, 0.18)
    return jnp.clip(entries, -limit, limit).astype(held_as)


def setup_inputs(seed: int = 0) -> dict:
    keys = jax.random.split(jax.random.key(seed), 14)
    mix_input = gaussian(keys[0], (TOKENS_MIX, D_POOL), 1.0, 6.0, ((0, 256),))
    pool_weight = gaussian(keys[1], (POOL_GROUPS, POOL_DIM, POOL_DIM), POOL_DIM ** -0.5, 0.5)
    pool_scale = jnp.clip(1.0 + 0.18 * jax.random.normal(keys[2], (D_POOL,), jnp.float32), 0.1, 1.9)
    out_weight = gaussian(keys[3], (D_POOL, D), D_POOL ** -0.5, 0.1875)
    moe_input = gaussian(keys[4], (TOKENS_MOE, D), 1.0, 6.0, ((0, 64),))
    moe_gain = jnp.clip(1.0 + 0.18 * jax.random.normal(keys[5], (D,), jnp.float32), 0.1, 1.9)
    group_router = gaussian(keys[6], (D, GROUPS), D ** -0.5, 0.125)
    inner_router = gaussian(keys[7], (D, EXPERTS), D ** -0.5, 0.125)
    group_pick = touch_ends(skewed_ids(keys[8], (TOKENS_MOE,), GROUPS, 2), jax.random.fold_in(keys[8], 3), 0, GROUPS - 1).astype(jnp.int32)
    inner_pick = distinct(keys[9], TOKENS_MOE, EPG, TOPK, 1024)
    gate_weight = gaussian(keys[10], (EXPERTS, D, FF), D ** -0.5, 0.125, ((0, 64), (2, 4)))
    up_weight = gaussian(keys[11], (EXPERTS, D, FF), D ** -0.5, 0.125, ((0, 64), (2, 4)))
    down_weight = gaussian(keys[12], (EXPERTS, FF, D), FF ** -0.5, 0.1875, ((0, 64), (1, 4)))
    return {"mix_input": mix_input, "pool_weight": pool_weight, "pool_scale": pool_scale, "out_weight": out_weight, "moe_input": moe_input, "moe_gain": moe_gain, "group_router": group_router, "inner_router": inner_router, "group_pick": group_pick, "inner_pick": inner_pick, "gate_weight": gate_weight, "up_weight": up_weight, "down_weight": down_weight}


NORM_FLOOR = 0.25

def trailing_means(padded, row_count, lead_rows):
    group_width = padded.shape[1] // 4
    position = jnp.arange(row_count, dtype=jnp.int32)
    pieces = []
    for scale_index in range(4):
        window = 2 ** (scale_index + 1)
        channel_block = padded[:, scale_index * group_width:(scale_index + 1) * group_width]
        window_sum = channel_block[lead_rows:lead_rows + row_count]
        for back_step in range(1, window):
            window_sum = window_sum + channel_block[lead_rows - back_step:lead_rows - back_step + row_count]
        divisor = jnp.minimum(position + 1, window).astype(jnp.float32)
        pieces.append(window_sum / divisor[:, None])
    return jnp.concatenate(pieces, axis=1)

def route_terms(group_logits, inner_logits, group_pick, inner_pick, per_group):
    group_ids = jnp.arange(group_logits.shape[1], dtype=jnp.int32)
    chosen = lax.optimization_barrier(jnp.sum(jnp.where(group_pick[:, None] == group_ids[None, :], group_logits, 0.0), axis=1))
    group_share = 1.0 / lax.optimization_barrier(jnp.sum(jnp.exp(group_logits - chosen[:, None]), axis=1))
    target = (group_pick[:, None] * per_group + inner_pick).astype(jnp.int32)
    expert_ids = jnp.arange(inner_logits.shape[1], dtype=jnp.int32)
    picked = lax.optimization_barrier(jnp.sum(jnp.where(target[:, :, None] == expert_ids[None, None, :], inner_logits[:, None, :], 0.0), axis=2))
    first_share = jax.nn.sigmoid(picked[:, 0] - picked[:, 1])
    route_weight = group_share[:, None] * jnp.stack([first_share, 1.0 - first_share], axis=1)
    return (target, route_weight)

def slot_terms(target, expert_count, capacity):
    expert_ids = jnp.arange(expert_count, dtype=jnp.int32)
    expert_hits = (target[:, :, None] == expert_ids[None, None, :]).astype(jnp.int32)
    per_token = lax.optimization_barrier(jnp.sum(expert_hits, axis=1))
    earlier = jnp.cumsum(per_token, axis=0) - per_token
    route_rank = lax.optimization_barrier(jnp.sum(expert_hits * earlier[:, None, :], axis=2))
    is_kept = route_rank < capacity
    slot_index = (target * capacity + jnp.minimum(route_rank, capacity - 1)).astype(jnp.int32)
    return (slot_index, is_kept)

def slot_sources(slot_index, is_kept, slot_count):
    token_ids = jnp.broadcast_to(jnp.arange(slot_index.shape[0], dtype=jnp.int32)[:, None], slot_index.shape)
    placed = jnp.where(is_kept, slot_index, slot_count).astype(jnp.int32).reshape(-1)
    source = jnp.zeros((slot_count,), jnp.int32).at[placed].set(token_ids.reshape(-1), mode='drop')
    slot_used = jnp.zeros((slot_count,), jnp.bool_).at[placed].set(True, mode='drop')
    return (source, slot_used)

def reference(mix_input, pool_weight, pool_scale, out_weight, moe_input, moe_gain, group_router, inner_router, group_pick, inner_pick, gate_weight, up_weight, down_weight):
    reach_back = WINDOW_MAX - 1
    row_count = mix_input.shape[0]
    values = mix_input.astype(jnp.float32)
    padded = jnp.concatenate([jnp.zeros((reach_back, values.shape[1]), jnp.float32), values], axis=0)
    trailing = trailing_means(padded, row_count, reach_back) - values
    pooled = trailing.astype(jnp.bfloat16)
    grouped = jnp.einsum('tgc,gcd->tgd', pooled.reshape(row_count, POOL_GROUPS, POOL_DIM).astype(jnp.float32), pool_weight.astype(jnp.float32))
    grouped = (grouped.reshape(row_count, D_POOL) * pool_scale[None, :]).astype(jnp.bfloat16)
    mix_out = jnp.dot(grouped, out_weight, preferred_element_type=jnp.float32).astype(jnp.bfloat16)
    token_values = moe_input.astype(jnp.float32)
    norm_scale = lax.rsqrt(jnp.maximum(lax.optimization_barrier(jnp.mean(token_values * token_values, axis=1, keepdims=True)), NORM_FLOOR))
    normed = (token_values * norm_scale * moe_gain[None, :]).astype(jnp.bfloat16)
    group_logits = jnp.dot(normed, group_router, preferred_element_type=jnp.float32)
    inner_logits = jnp.dot(normed, inner_router, preferred_element_type=jnp.float32)
    target, route_weight = route_terms(group_logits, inner_logits, group_pick, inner_pick, EPG)
    block_target = target.reshape(N_EP, TOK_MOE, TOPK)

    def block_slots(one_block):
        return slot_terms(one_block, EXPERTS, CAP)
    slot_index, is_kept = lax.map(block_slots, block_target)

    def block_sources(pair):
        return slot_sources(pair[0], pair[1], EXPERTS * CAP)
    source, slot_used = lax.map(block_sources, (slot_index, is_kept))
    global_source = source + (jnp.arange(N_EP, dtype=jnp.int32) * TOK_MOE)[:, None]
    by_expert = global_source.reshape(N_EP, EXPERTS, CAP).transpose(1, 0, 2).reshape(EXPERTS, N_EP * CAP)
    used_by_expert = slot_used.reshape(N_EP, EXPERTS, CAP).transpose(1, 0, 2).reshape(EXPERTS, N_EP * CAP)

    def run_expert(items):
        token_rows, row_used, gate_matrix, up_matrix, down_matrix = items
        expert_rows = jnp.where(row_used[:, None], normed[token_rows], jnp.zeros((), jnp.bfloat16))
        gate_sum = jnp.dot(expert_rows, gate_matrix, preferred_element_type=jnp.float32)
        up_sum = jnp.dot(expert_rows, up_matrix, preferred_element_type=jnp.float32)
        hidden = (jax.nn.silu(gate_sum) * up_sum).astype(jnp.bfloat16)
        result_sum = jnp.zeros((expert_rows.shape[0], D), jnp.float32)
        for part_index in range(N_TP):
            part_product = jnp.dot(hidden[:, part_index * FF_PART:(part_index + 1) * FF_PART], down_matrix[part_index * FF_PART:(part_index + 1) * FF_PART], preferred_element_type=jnp.float32).astype(jnp.bfloat16)
            result_sum = result_sum + lax.optimization_barrier(part_product).astype(jnp.float32)
        return result_sum.astype(jnp.bfloat16)
    results = lax.map(run_expert, (by_expert, used_by_expert, gate_weight, up_weight, down_weight))
    results = results.reshape(EXPERTS, N_EP, CAP, D)
    flat_slot = slot_index.reshape(TOKENS_MOE, TOPK)
    flat_kept = is_kept.reshape(TOKENS_MOE, TOPK)
    rank_of = (flat_slot - target * CAP).astype(jnp.int32)
    block_of = (jnp.arange(TOKENS_MOE, dtype=jnp.int32) // TOK_MOE)[:, None]
    picked = results[target, block_of, rank_of]
    route_scale = jnp.where(flat_kept, route_weight, 0.0).astype(jnp.bfloat16)
    route_scale = lax.optimization_barrier(route_scale).astype(jnp.float32)
    moe_out = lax.optimization_barrier(jnp.sum(picked.astype(jnp.float32) * route_scale[:, :, None], axis=1)).astype(jnp.bfloat16)
    return (mix_out, moe_out)
```

```python
import functools

import jax
import jax.numpy as jnp
from jax import lax
from jax.experimental import pallas as pl
from jax.experimental.pallas import tpu as pltpu
from jax.sharding import PartitionSpec as P

MESH = pl.DeviceIdType.MESH
NORM_FLOOR = 0.25
WINDOW_MAX = 16
HALO = 16
CAP = 8
PLANE = 8
F32 = jnp.float32
BF16 = jnp.bfloat16

SKEW_FORWARD = 1
SKEW_EXPERT = 2
SKEW_OPPOSITE = 3
SKEW_OWNER = 4


def kernel(
    n_ep,
    n_tp,
    mix_hbm,
    pool_hbm,
    pscale_hbm,
    outw_hbm,
    moe_hbm,
    gain_hbm,
    group_router_hbm,
    inner_router_hbm,
    group_pick_hbm,
    inner_pick_hbm,
    gate_hbm,
    up_hbm,
    down_hbm,
    mix_out,
    moe_out,
    mix_in,
    halo,
    pool_w,
    pscale,
    out_w,
    grouped,
    moe_in,
    gain,
    group_router,
    inner_router,
    group_pick,
    inner_pick,
    gate_w,
    up_w,
    down_w,
    normed,
    outgoing,
    arrived,
    partial,
    opp_left,
    opp_right,
    own_left,
    own_right,
    result,
    returned,
    spread_t,
    load_sem,
    own_sem,
    halo_send,
    halo_recv,
    disp_send,
    disp_recv,
    ag_send,
    ag_recv,
    rs_send,
    rs_recv,
    ret_send,
    ret_recv,
):
    n_planes = n_ep // PLANE
    half = PLANE // 2
    e = lax.axis_index("ep")
    t = lax.axis_index("tp")
    right, left = lax.rem(t + 1, n_tp), lax.rem(t + n_tp - 1, n_tp)
    opposite = lax.rem(t + 2, n_tp)
    plane = lax.div(e, PLANE)
    seat = lax.rem(e, PLANE)
    linear = e * n_tp + t
    n_all = n_ep * n_tp
    after = lax.rem(linear + 1, n_all)
    before = lax.rem(linear + n_all - 1, n_all)

    barrier = pltpu.get_barrier_semaphore()

    @pl.loop(1, n_ep)
    def _(step):
        pl.semaphore_signal(
            barrier, inc=1, device_id=(lax.rem(e + step, n_ep), t), device_id_type=MESH
        )

    for other in (right, left, opposite):
        pl.semaphore_signal(barrier, inc=1, device_id=(e, other), device_id_type=MESH)
    pl.semaphore_signal(
        barrier,
        inc=1,
        device_id=(lax.div(before, n_tp), lax.rem(before, n_tp)),
        device_id_type=MESH,
    )

    loads = [
        (group_pick_hbm, group_pick),
        (inner_pick_hbm, inner_pick),
        (moe_hbm, moe_in),
        (gain_hbm, gain),
        (mix_hbm, mix_in),
        (pool_hbm, pool_w),
        (pscale_hbm, pscale),
        (gate_hbm, gate_w),
        (up_hbm, up_w),
        (down_hbm, down_w),
        (outw_hbm, out_w),
        (inner_router_hbm, inner_router),
        (group_router_hbm, group_router),
    ]
    loads = [
        pltpu.make_async_copy(source, target, load_sem.at[index])
        for index, (source, target) in enumerate(loads)
    ]
    for load in loads:
        load.start()
    for load in loads[:4]:
        load.wait()

    n_tok = moe_in.shape[0]
    n_slot = n_ep * CAP
    group_row = group_pick[...]
    first = group_row * (n_ep // 4) + inner_pick[0:1, :]
    second = group_row * (n_ep // 4) + inner_pick[1:2, :]
    expert_row = lax.broadcasted_iota(jnp.int32, (n_ep, n_tok), 0)
    hit = (expert_row == first) | (expert_row == second)
    earlier_than = lax.broadcasted_iota(jnp.int32, (n_tok, n_tok), 0) < lax.broadcasted_iota(
        jnp.int32, (n_tok, n_tok), 1
    )
    hit_count = jnp.where(hit, 1.0, 0.0).astype(BF16)
    rank = jnp.dot(hit_count, jnp.where(earlier_than, 1.0, 0.0).astype(BF16), preferred_element_type=F32)
    rank = jnp.where(hit, rank, -1.0)
    slot_row = lax.broadcasted_iota(jnp.int32, (n_slot, n_ep), 0)
    slot_expert = lax.broadcasted_iota(jnp.int32, (n_slot, n_ep), 1) * CAP
    to_slot = jnp.where((slot_row >= slot_expert) & (slot_row < slot_expert + CAP), 1.0, 0.0).astype(BF16)
    slot_rank = jnp.dot(to_slot, rank.astype(BF16), preferred_element_type=F32)
    want_rank = lax.rem(lax.broadcasted_iota(jnp.int32, (n_slot, n_tok), 0), CAP).astype(F32)
    spread = jnp.where(slot_rank == want_rank, 1.0, 0.0)

    values = moe_in[...].astype(F32)
    scale = lax.rsqrt(jnp.maximum(jnp.mean(values * values, axis=1, keepdims=True), NORM_FLOOR))
    normed[...] = (values * scale * gain[...]).astype(BF16)
    width = outgoing.shape[2]
    own_columns = normed[:, pl.ds(pl.multiple_of(t * width, width), width)]
    outgoing[...] = (
        jnp.dot(spread.astype(BF16), own_columns, preferred_element_type=F32)
        .reshape(n_ep, CAP, width)
        .astype(BF16)
    )

    pl.semaphore_wait(barrier, n_ep - 1 + 3 + 1)

    def plane_at(step):
        size = lax.div(step + 1, 2)
        return size * (2 * lax.rem(step, 2) - 1)

    def source_plane(step):
        return lax.rem(plane - plane_at(step) + n_planes, n_planes)

    def target_plane(step):
        return lax.rem(plane + plane_at(step) + n_planes, n_planes)

    own_copy = pltpu.make_async_copy(outgoing.at[e], arrived.at[t, e], own_sem.at[0])
    own_copy.start()

    def send_block(step, peer):
        pltpu.make_async_remote_copy(
            src_ref=outgoing.at[peer],
            dst_ref=arrived.at[t, e],
            send_sem=disp_send,
            recv_sem=disp_recv.at[step],
            device_id=(peer, t),
            device_id_type=MESH,
        ).start()

    @pl.loop(1, PLANE)
    def _(turn):
        send_block(0, plane * PLANE + lax.rem(seat + turn, PLANE))

    @pl.loop(1, n_planes)
    def _(step):
        @pl.loop(0, PLANE)
        def _(turn):
            send_block(step, target_plane(step) * PLANE + lax.rem(seat + turn, PLANE))

    halo_copy = pltpu.make_async_remote_copy(
        src_ref=mix_hbm.at[pl.ds(mix_hbm.shape[0] - HALO, HALO)],
        dst_ref=halo,
        send_sem=halo_send,
        recv_sem=halo_recv,
        device_id=(lax.div(after, n_tp), lax.rem(after, n_tp)),
        device_id_type=MESH,
    )
    halo_copy.start()

    def to_neighbour(ref, target, send_sem, recv_sem, side):
        return pltpu.make_async_remote_copy(
            src_ref=ref,
            dst_ref=target,
            send_sem=send_sem,
            recv_sem=recv_sem,
            device_id=(e, side),
            device_id_type=MESH,
        )

    def drain(ref, sem):
        pltpu.make_async_copy(ref, ref, sem).wait()

    def rows_of(step):
        return source_plane(step) * PLANE

    def share(step):
        base = rows_of(step)
        block = arrived.at[t, pl.ds(base, PLANE)]

        @pl.when(step == 0)
        def _():
            own_copy.wait()
            drain(arrived.at[t, pl.ds(base, PLANE - 1)], disp_recv.at[step])

        @pl.when(step > 0)
        def _():
            drain(block, disp_recv.at[step])

        to_neighbour(block, block, ag_send.at[0], ag_recv.at[0, step], right).start()
        to_neighbour(block, block, ag_send.at[1], ag_recv.at[1, step], left).start()

    def forward(step):
        base = rows_of(step)
        drain(arrived.at[left, pl.ds(base, PLANE)], ag_recv.at[0, step])
        block = arrived.at[left, pl.ds(base, half)]
        to_neighbour(block, block, ag_send.at[2], ag_recv.at[2, step], right).start()
        drain(arrived.at[right, pl.ds(base, PLANE)], ag_recv.at[1, step])
        block = arrived.at[right, pl.ds(base + half, half)]
        to_neighbour(block, block, ag_send.at[3], ag_recv.at[3, step], left).start()

    def run_expert(step):
        base = rows_of(step)
        drain(arrived.at[opposite, pl.ds(base, half)], ag_recv.at[2, step])
        drain(arrived.at[opposite, pl.ds(base, half)], ag_recv.at[3, step])
        gate_sum, up_sum = 0.0, 0.0
        for piece in range(n_tp):
            rows = arrived[piece, pl.ds(base, PLANE)].reshape(PLANE * CAP, width)
            part = pl.ds(piece * width, width)
            gate_sum += jnp.dot(rows, gate_w[part, :], preferred_element_type=F32)
            up_sum += jnp.dot(rows, up_w[part, :], preferred_element_type=F32)
        hidden = (gate_sum / (1.0 + jnp.exp(-gate_sum)) * up_sum).astype(BF16)
        for piece in range(n_tp):
            product = jnp.dot(
                hidden, down_w[:, piece * width : (piece + 1) * width], preferred_element_type=F32
            )
            partial[piece, pl.ds(base, PLANE)] = product.reshape(PLANE, CAP, width).astype(BF16)
        to_neighbour(
            partial.at[opposite, pl.ds(base, half)],
            opp_left.at[step],
            rs_send.at[0],
            rs_recv.at[0, step],
            right,
        ).start()
        to_neighbour(
            partial.at[opposite, pl.ds(base + half, half)],
            opp_right.at[step],
            rs_send.at[1],
            rs_recv.at[1, step],
            left,
        ).start()

    def add_opposite(step):
        base = rows_of(step)
        for lane, (slot, start, side, target) in enumerate(
            (
                (opp_left, base, right, own_left),
                (opp_right, base + half, left, own_right),
            )
        ):
            drain(slot.at[step], rs_recv.at[lane, step])
            rows = pl.ds(start, half)
            partial[side, rows] = (partial[side, rows].astype(F32) + slot[step].astype(F32)).astype(BF16)
            to_neighbour(
                partial.at[side, pl.ds(base, PLANE)],
                target.at[step],
                rs_send.at[2 + lane],
                rs_recv.at[2 + lane, step],
                side,
            ).start()

    def finish(step):
        base = rows_of(step)
        drain(own_left.at[step], rs_recv.at[2, step])
        drain(own_right.at[step], rs_recv.at[3, step])
        rows = pl.ds(base, PLANE)
        result[rows] = (
            partial[t, rows].astype(F32) + own_left[step].astype(F32) + own_right[step].astype(F32)
        ).astype(BF16)

        def give_back(turn):
            peer = base + lax.rem(seat + turn, PLANE)
            pltpu.make_async_remote_copy(
                src_ref=result.at[peer],
                dst_ref=returned.at[e],
                send_sem=ret_send,
                recv_sem=ret_recv.at[step],
                device_id=(peer, t),
                device_id_type=MESH,
            ).start()

        @pl.when(step == 0)
        def _():
            pltpu.make_async_copy(result.at[e], returned.at[e], own_sem.at[1]).start()

            @pl.loop(1, PLANE)
            def _(turn):
                give_back(turn)

        @pl.when(step > 0)
        def _():
            @pl.loop(0, PLANE)
            def _(turn):
                give_back(turn)

    rows_mix = mix_in.shape[0]

    def pool():
        halo_copy.wait()
        for load in loads[4:7]:
            load.wait()
        lead = jnp.where(linear > 0, halo[...].astype(F32), 0.0)
        position = linear * rows_mix + lax.broadcasted_iota(jnp.int32, (rows_mix, 1), 0)
        scale_width = mix_in.shape[1] // 4
        pool_dim = pool_w.shape[1]
        for index in range(4):
            columns = slice(index * scale_width, (index + 1) * scale_width)
            own = mix_in[:, columns].astype(F32)
            total = jnp.concatenate([lead[:, columns], own], axis=0)
            for doubling in range(index + 1):
                total = total + pltpu.roll(total, 2**doubling, 0)
            divisor = jnp.minimum(position + 1, 2 ** (index + 1)).astype(F32)
            pooled = (total[HALO:] / divisor - own).astype(BF16)
            for part in range(scale_width // pool_dim):
                group = index * (scale_width // pool_dim) + part
                product = jnp.dot(
                    pooled[:, part * pool_dim : (part + 1) * pool_dim],
                    pool_w[group],
                    preferred_element_type=F32,
                )
                span = slice(group * pool_dim, (group + 1) * pool_dim)
                grouped[:, span] = (product * pscale[:, span]).astype(BF16)
        loads[10].wait()

    def project(piece):
        columns = pl.ds(pl.multiple_of(piece * width, width), width)
        mix_out[:, columns] = jnp.dot(
            grouped[...], out_w[:, columns], preferred_element_type=F32
        ).astype(BF16)

    pool()
    for load in loads[7:10]:
        load.wait()

    @pl.loop(0, n_planes + SKEW_OWNER)
    def _(now):
        def at(skew, stage):
            @pl.when((now >= skew) & (now < n_planes + skew))
            def _():
                stage(now - skew)

        at(0, share)
        at(SKEW_FORWARD, forward)
        at(SKEW_EXPERT, run_expert)
        at(SKEW_OPPOSITE, add_opposite)
        at(SKEW_OWNER, finish)

        @pl.when(now < 4)
        def _():
            project(now)

    for load in loads[11:]:
        load.wait()
    contract_last = (((1,), (1,)), ((), ()))
    group_logits = lax.dot_general(
        group_router[...], normed[...], contract_last, preferred_element_type=F32
    )
    inner_logits = lax.dot_general(
        inner_router[...], normed[...], contract_last, preferred_element_type=F32
    )
    group_ids = lax.broadcasted_iota(jnp.int32, group_logits.shape, 0)
    chosen = jnp.sum(jnp.where(group_ids == group_row, group_logits, 0.0), axis=0, keepdims=True)
    group_share = 1.0 / jnp.sum(jnp.exp(group_logits - chosen), axis=0, keepdims=True)
    picked_first = jnp.sum(jnp.where(expert_row == first, inner_logits, 0.0), axis=0, keepdims=True)
    picked_second = jnp.sum(jnp.where(expert_row == second, inner_logits, 0.0), axis=0, keepdims=True)
    first_share = jax.nn.sigmoid(picked_first - picked_second)
    route_weight = jnp.where(
        expert_row == first,
        group_share * first_share,
        jnp.where(expert_row == second, group_share * (1.0 - first_share), 0.0),
    )
    slot_weight = jnp.dot(to_slot, route_weight.astype(BF16), preferred_element_type=F32)
    spread_t[...] = jnp.transpose(spread * slot_weight).astype(BF16)

    pltpu.make_async_copy(result.at[e], returned.at[e], own_sem.at[1]).wait()
    drain(returned.at[pl.ds(0, PLANE - 1)], ret_recv.at[0])

    @pl.loop(1, n_planes)
    def _(step):
        drain(returned.at[pl.ds(0, PLANE)], ret_recv.at[step])

    moe_out[...] = jnp.dot(
        spread_t[...], returned[...].reshape(n_slot, width), preferred_element_type=F32
    ).astype(BF16)

    drain(outgoing.at[pl.ds(0, n_ep - 1)], disp_send)
    drain(result.at[pl.ds(0, n_ep - 1)], ret_send)
    for lane, ref in enumerate((returned, returned, opp_left, opp_right)):
        drain(ref, ag_send.at[lane])
    for lane, ref in enumerate((opp_left, opp_right, own_left, own_right)):
        drain(ref, rs_send.at[lane])


def per_device(
    n_ep,
    n_tp,
    mix_input,
    pool_weight,
    pool_scale,
    out_weight,
    moe_input,
    moe_gain,
    group_router,
    inner_router,
    group_pick,
    inner_pick,
    gate_weight,
    up_weight,
    down_weight,
):
    rows, channels = mix_input.shape
    tokens, features = moe_input.shape
    width = features // n_tp
    hidden = gate_weight.shape[2]
    n_planes = n_ep // PLANE
    half = PLANE // 2
    operands = (
        mix_input,
        pool_weight,
        pool_scale.reshape(1, -1),
        out_weight,
        moe_input,
        moe_gain.reshape(1, -1),
        group_router.T,
        inner_router.T,
        group_pick.reshape(1, -1),
        inner_pick.T,
        gate_weight[0],
        up_weight[0],
        down_weight[0],
    )

    def like(array):
        return pltpu.VMEM(array.shape, array.dtype)

    (mix, pool, pscale, outw, moe, gain, grouter, irouter, gpick, ipick, gate, up, down) = operands
    slots = pltpu.VMEM((n_ep, CAP, width), BF16)
    by_step = pltpu.VMEM((n_planes, PLANE, CAP, width), BF16)
    half_step = pltpu.VMEM((n_planes, half, CAP, width), BF16)
    dma = pltpu.SemaphoreType.DMA
    return pl.pallas_call(
        functools.partial(kernel, n_ep, n_tp),
        out_shape=(
            jax.ShapeDtypeStruct((rows, outw.shape[1]), BF16),
            jax.ShapeDtypeStruct((tokens, width), BF16),
        ),
        in_specs=[pl.BlockSpec(memory_space=pl.ANY)] * len(operands),
        out_specs=(pl.BlockSpec(memory_space=pltpu.VMEM), pl.BlockSpec(memory_space=pltpu.VMEM)),
        scratch_shapes=[
            like(mix),
            pltpu.VMEM((HALO, channels), BF16),
            like(pool),
            like(pscale),
            like(outw),
            pltpu.VMEM((rows, channels), BF16),
            like(moe),
            like(gain),
            like(grouter),
            like(irouter),
            like(gpick),
            like(ipick),
            like(gate),
            like(up),
            like(down),
            pltpu.VMEM((tokens, features), BF16),
            slots,
            pltpu.VMEM((n_tp, n_ep, CAP, width), BF16),
            pltpu.VMEM((n_tp, n_ep, CAP, width), BF16),
            half_step,
            half_step,
            by_step,
            by_step,
            slots,
            slots,
            pltpu.VMEM((tokens, n_ep * CAP), BF16),
            dma((len(operands),)),
            dma((2,)),
            dma,
            dma,
            dma,
            dma((n_planes,)),
            dma((4,)),
            dma((4, n_planes)),
            dma((4,)),
            dma((4, n_planes)),
            dma,
            dma((n_planes,)),
        ],
        compiler_params=pltpu.CompilerParams(collective_id=0, has_side_effects=True),
    )(*operands)


def solution(mesh):
    in_specs = (
        P(("ep", "tp"), None),
        P(),
        P(),
        P(),
        P("ep", None),
        P(),
        P(),
        P(),
        P("ep"),
        P("ep", None),
        P("ep", None, "tp"),
        P("ep", None, "tp"),
        P("ep", "tp", None),
    )
    out_specs = (P(("ep", "tp"), None), P("ep", "tp"))
    return jax.shard_map(
        functools.partial(per_device, mesh.shape["ep"], mesh.shape["tp"]),
        mesh=mesh,
        in_specs=in_specs,
        out_specs=out_specs,
        check_vma=False,
    )
```
